32 devices in a mesh: grp: 2 (over x), ep: 16 (over z, y, core).
Axes of the slice: x: 2, y: 2, z: 4, core: 2. Of those that a mesh axis runs over, the one named last changes fastest.
Arguments:
- residual: bfloat16 [16, 4096], P('grp', 'ep'), parts along dimension 0, may hold values from -6 to 6
- head_states: float32 [64, 512, 1024], P(('grp', 'ep')), parts along dimension 0, may hold values from -6 to 6
- first_gain: bfloat16 [4096], replicated, may hold values from 0.099609375 to 1.8984375
- w_query: bfloat16 [4096, 2048], P(None, 'ep'), may hold values from -0.09375 to 0.09375
- w_key: bfloat16 [4096, 2048], P(None, 'ep'), may hold values from -0.09375 to 0.09375
- w_value: bfloat16 [4096, 4096], P(None, 'ep'), may hold values from -0.09375 to 0.09375
- w_gate: bfloat16 [4096, 4096], P(None, 'ep'), may hold values from -0.09375 to 0.09375
- w_low: bfloat16 [4096, 16], replicated, may hold values from -0.09375 to 0.09375
- w_decay: bfloat16 [16, 2048], replicated, may hold values from -15 to 15
- decay_bias: float32 [2048], replicated, may hold values from -40 to 4
- head_gain: bfloat16 [1024], replicated, may hold values from 0.099609375 to 1.8984375
- w_output: bfloat16 [4096, 4096], P(None, 'ep'), may hold values from -0.09375 to 0.09375
- second_gain: bfloat16 [4096], replicated, may hold values from 0.099609375 to 1.8984375
- routes: int32 [16, 2], P('grp'), parts along dimension 0, may hold values from 0 to 15, as said below
- group_logits: float32 [16, 4], P('grp'), parts along dimension 0, may hold values from -12 to 12
- expert_logits: float32 [16, 2], P('grp'), parts along dimension 0, may hold values from -9 to 9
- expert_gate: bfloat16 [16, 4096, 512], P('ep'), may hold values from -0.09375 to 0.09375
- expert_up: bfloat16 [16, 4096, 512], P('ep'), may hold values from -0.09375 to 0.09375
- expert_down: bfloat16 [16, 512, 4096], P('ep'), may hold values from -0.25 to 0.25
Outputs:
- layer_out: bfloat16 [16, 4096], P('grp', 'ep'), parts along dimension 0
- new_states: float32 [64, 512, 1024], P(('grp', 'ep')), parts along dimension 0
The draws below stay inside these ranges and needn't reach their ends.
There are 2 independent parts, one for each index of `grp`. The reference program is written for one: setup_inputs(seed, part) draws one part's arguments, and reference() takes and returns one part's arrays. A program takes and returns all parts, laid end to end along the dimension named above; an argument that names none is the same for every part. Nothing has to cross between parts.
Inputs may be any that keep to these rules, and one draw needn't show every extreme that they name: `routes`: each row names 2 different experts of one group (numbers g * 4 to g * 4 + 3). No expert is named by more than 2 rows, and in every draw all experts of one group are named by exactly 2 rows.
All inputs are finite; a program needn't handle non-finite values.
Results may differ from the reference program's by a relative error of at most 0.014.
Values may be sent and summed in bfloat16 or wider, within the bound.
A program may use at most 128 MiB of HBM per device.

```python
import jax
import jax.numpy as jnp
from jax import lax

D = 4096
HEADS = 4
DK = 512
DV = 1024
RANK = 16
FF = 512
GROUPS = 4
TOP = 2
SEQS = 8
PAIRS = 32
EXPERTS = 16
EPG = 4
CAP = 2


def draw_routes(key, part):
    order_key, full_key, other_key, perm_key = jax.random.split(jax.random.fold_in(key, 17), 4)
    full_count = EPG * CAP // TOP
    order = jax.random.permutation(order_key, SEQS)
    full_group = jax.random.randint(full_key, (), 0, GROUPS, dtype=jnp.int32)
    others = jax.random.randint(other_key, (SEQS,), 0, GROUPS - 1, dtype=jnp.int32)
    others = others + (others >= full_group).astype(jnp.int32)
    position = jnp.arange(SEQS, dtype=jnp.int32)
    by_position = jnp.where(position < full_count, full_group, others)
    group = jnp.zeros((SEQS,), jnp.int32).at[order].set(by_position)
    member = (group[:, None] == jnp.arange(GROUPS, dtype=jnp.int32)[None, :]).astype(jnp.int32)
    before = jnp.cumsum(member, axis=0) - member
    rank = jnp.sum(before * member, axis=1)
    tables = jax.vmap(lambda one: jax.random.permutation(one, EPG))(jax.random.split(perm_key, GROUPS)).astype(jnp.int32)
    slots = TOP * rank[:, None] + jnp.arange(TOP, dtype=jnp.int32)[None, :]
    local = slots % EPG
    chosen = tables[group[:, None], local]
    return (group[:, None] * EPG + chosen).astype(jnp.int32)


def steps_of(own_key, dims, pieces, low, largest):
    factor_of, own = 1.0, jax.random.fold_in(own_key, 6)
    for dim, parts in pieces:
        steps = jnp.exp(jax.random.uniform(jax.random.fold_in(own, dim), (parts,), jnp.float32, low / len(pieces), largest / len(pieces)))
        factor_of = factor_of * jnp.repeat(steps, dims[dim] // parts).reshape([-1 if axis == dim else 1 for axis in range(len(dims))])
    return factor_of


def gaussian(rng, extent, scale, bound, cuts=(), held_as=jnp.bfloat16):
    level = steps_of(rng, extent, cuts, -0.22, 0.18) if cuts else 1.0
    array = jax.random.normal(rng, extent, jnp.float32) * scale * level
    return jnp.minimum(jnp.maximum(array, -bound), bound).astype(held_as)


def setup_inputs(seed: int = 0, part: int = 0) -> dict:
    arg_keys = jax.random.split(jax.random.key(seed), 20)
    part_splits = jax.random.split(jax.random.fold_in(arg_keys[19], part), 20)
    return {
        "residual": gaussian(part_splits[0], (SEQS, D), 1.0, 6.0, ((1, 16),)),
        "head_states": gaussian(part_splits[1], (PAIRS, DK, DV), 1.0, 6.0, ((0, 16),), jnp.float32),
        "first_gain": jnp.clip(1.0 + 0.18 * jax.random.normal(arg_keys[2], (D,), jnp.float32), 0.099609375, 1.8984375).astype(jnp.bfloat16),
        "w_query": gaussian(arg_keys[3], (D, HEADS * DK), D ** -0.5, 0.09375, ((1, 16),)),
        "w_key": gaussian(arg_keys[4], (D, HEADS * DK), D ** -0.5, 0.09375, ((1, 16),)),
        "w_value": gaussian(arg_keys[5], (D, HEADS * DV), D ** -0.5, 0.09375, ((1, 16),)),
        "w_gate": gaussian(arg_keys[6], (D, HEADS * DV), D ** -0.5, 0.09375, ((1, 16),)),
        "w_low": gaussian(arg_keys[7], (D, RANK), D ** -0.5, 0.09375),
        "w_decay": gaussian(arg_keys[8], (RANK, HEADS * DK), 3.0, 15.0),
        "decay_bias": jnp.clip(jax.random.uniform(arg_keys[9], (HEADS * DK,), jnp.float32, -40.0, 4.0), -40.0, 4.0),
        "head_gain": jnp.clip(1.0 + 0.18 * jax.random.normal(arg_keys[10], (DV,), jnp.float32), 0.099609375, 1.8984375).astype(jnp.bfloat16),
        "w_output": gaussian(arg_keys[11], (HEADS * DV, D), (HEADS * DV) ** -0.5, 0.09375, ((1, 16),)),
        "second_gain": jnp.clip(1.0 + 0.18 * jax.random.normal(arg_keys[12], (D,), jnp.float32), 0.099609375, 1.8984375).astype(jnp.bfloat16),
        "routes": draw_routes(jax.random.fold_in(jax.random.fold_in(arg_keys[19], part), 71), part),
        "group_logits": gaussian(part_splits[14], (SEQS, GROUPS), 2.0, 12.0, (), jnp.float32),
        "expert_logits": gaussian(part_splits[15], (SEQS, TOP), 1.5, 9.0, (), jnp.float32),
        "expert_gate": gaussian(arg_keys[16], (EXPERTS, D, FF), D ** -0.5, 0.09375, ((0, 16),)),
        "expert_up": gaussian(arg_keys[17], (EXPERTS, D, FF), D ** -0.5, 0.09375, ((0, 16),)),
        "expert_down": gaussian(arg_keys[18], (EXPERTS, FF, D), FF ** -0.5, 0.25, ((0, 16),)),
    }


norm_eps = 1e-06
decay_tau = 16.0

def rms_scale(values, gain):
    floats = values.astype(jnp.float32)
    return floats * lax.rsqrt(lax.optimization_barrier(jnp.mean(floats * floats, axis=-1, keepdims=True)) + norm_eps) * gain.astype(jnp.float32)

def route_weights(routes, group_logits, expert_logits, per_group):
    group_exp = jnp.exp(group_logits)
    group_prob = group_exp / lax.optimization_barrier(jnp.sum(group_exp, axis=1, keepdims=True))
    chosen = routes[:, 0] // per_group
    groups_row = jnp.arange(group_logits.shape[1], dtype=jnp.int32)
    picked = lax.optimization_barrier(jnp.sum(group_prob * (chosen[:, None] == groups_row[None, :]).astype(jnp.float32), axis=1))
    expert_exp = jnp.exp(expert_logits)
    return expert_exp / lax.optimization_barrier(jnp.sum(expert_exp, axis=1, keepdims=True)) * picked[:, None]

def reference(residual, head_states, first_gain, w_query, w_key, w_value, w_gate, w_low, w_decay, decay_bias, head_gain, w_output, second_gain, routes, group_logits, expert_logits, expert_gate, expert_up, expert_down):
    normed = rms_scale(residual, first_gain).astype(jnp.bfloat16)
    query = jnp.dot(normed, w_query, preferred_element_type=jnp.float32).astype(jnp.bfloat16).reshape(PAIRS, DK)
    key = jnp.dot(normed, w_key, preferred_element_type=jnp.float32).astype(jnp.bfloat16).reshape(PAIRS, DK)
    value = jnp.dot(normed, w_value, preferred_element_type=jnp.float32).astype(jnp.bfloat16).reshape(PAIRS, DV)
    gate = jnp.dot(normed, w_gate, preferred_element_type=jnp.float32).astype(jnp.bfloat16).reshape(PAIRS, DV)
    low = jnp.dot(normed, w_low, preferred_element_type=jnp.float32)
    decay_pre = jnp.dot(low, w_decay.astype(jnp.float32), precision=lax.Precision.HIGHEST) + decay_bias
    log_decay = jax.nn.log_sigmoid(decay_pre.reshape(PAIRS, DK)) / decay_tau
    new_states = head_states * jnp.exp(log_decay)[:, :, None] + key.astype(jnp.float32)[:, :, None] * value.astype(jnp.float32)[:, None, :]
    read = jnp.einsum('pk,pkv->pv', query.astype(jnp.float32) * DK ** (-0.5), new_states, precision=lax.Precision.HIGHEST)
    mixed = (rms_scale(read, head_gain) * jax.nn.silu(gate.astype(jnp.float32))).astype(jnp.bfloat16)
    branch = jnp.dot(mixed.reshape(SEQS, HEADS * DV), w_output, preferred_element_type=jnp.float32).astype(jnp.bfloat16)
    stream = (residual.astype(jnp.float32) + branch.astype(jnp.float32)).astype(jnp.bfloat16)
    expert_in = rms_scale(stream, second_gain).astype(jnp.bfloat16)
    weights = route_weights(routes, group_logits, expert_logits, EPG)
    every = jnp.arange(EXPERTS, dtype=jnp.int32)
    combine = lax.optimization_barrier(jnp.sum(weights[:, :, None] * (routes[:, :, None] == every[None, None, :]).astype(jnp.float32), axis=1))

    def one_expert(total, inputs):
        gate_w, up_w, down_w, share = inputs
        gate_part = jnp.dot(expert_in, gate_w, preferred_element_type=jnp.float32)
        up_part = jnp.dot(expert_in, up_w, preferred_element_type=jnp.float32)
        active = (jax.nn.silu(gate_part) * up_part * share[:, None]).astype(jnp.bfloat16)
        contribution = jnp.dot(active, down_w, preferred_element_type=jnp.float32).astype(jnp.bfloat16)
        return (total + contribution.astype(jnp.float32), None)
    start = jnp.zeros((SEQS, D), jnp.float32)
    summed, _ = lax.scan(one_expert, start, (expert_gate, expert_up, expert_down, combine.T))
    layer_out = (stream.astype(jnp.float32) + summed).astype(jnp.bfloat16)
    return (layer_out, new_states)
```

```python
import functools

import jax
import jax.numpy as jnp
from jax import lax
from jax.experimental import pallas as pl
from jax.experimental.pallas import tpu as pltpu
from jax.sharding import PartitionSpec as P

HEADS = 4
DK = 512
DV = 1024
GROUPS = 4

NORM_EPS = 1e-06
DECAY_TAU = 16.0
MESH = pl.DeviceIdType.MESH
F32 = jnp.float32
BF16 = jnp.bfloat16


def kernel_body(n, *refs):
    (
        residual,
        head_states,
        first_gain,
        w_query,
        w_key,
        w_value,
        w_gate,
        w_low,
        w_decay,
        decay_bias,
        head_gain,
        w_output,
        second_gain,
        routes,
        group_logits,
        expert_logits,
        expert_gate,
        expert_up,
        expert_down,
        layer_out,
        new_states,
        res_v,
        states_v,
        gain1_v,
        wq_v,
        wk_v,
        wv_v,
        wg_v,
        wlow_v,
        wdec_v,
        bias_v,
        hgain_v,
        wout_v,
        gain2_v,
        routes_v,
        glog_v,
        elog_v,
        eg_v,
        eu_v,
        ed_v,
        gath1,
        lhs,
        send2,
        recv2,
        cols,
        send3,
        gath3,
        stage3,
        stream_v,
        gath4,
        send5,
        recv5,
        out_v,
        local_sem,
        out_sem,
        s1,
        r1,
        s2,
        r2,
        s3,
        r3,
        s4,
        r4,
        s5,
        r5,
    ) = refs
    me = lax.axis_index("ep")
    seqs, own = residual.shape
    width = own * n
    pairs_dev = head_states.shape[0]
    dph = n // HEADS
    qw, vw = w_query.shape[1], w_value.shape[1]
    group_src = pairs_dev * dph
    my_seq = me * pairs_dev // HEADS
    my_head0 = lax.rem(me * pairs_dev, HEADS)
    src_head = me // dph
    tiles2 = send2.shape[1]
    rows3 = send3.shape[0]

    pieces = [
        (residual, res_v),
        (first_gain, gain1_v),
        (w_query, wq_v),
        (w_key, wk_v),
        (w_value, wv_v),
        (w_gate, wg_v),
        (w_low, wlow_v),
        (w_decay, wdec_v),
        (decay_bias, bias_v),
        (head_states, states_v),
        (head_gain, hgain_v),
        (w_output, wout_v),
        (second_gain, gain2_v),
        (routes, routes_v),
        (group_logits, glog_v),
        (expert_logits, elog_v),
        (expert_gate, eg_v),
        (expert_up, eu_v),
        (expert_down, ed_v),
    ]
    copies = [
        pltpu.make_async_copy(src, dst, local_sem.at[i]) for i, (src, dst) in enumerate(pieces)
    ]
    for copy in copies:
        copy.start()

    def staged(*indices):
        for i in indices:
            copies[i].wait()

    barrier = pltpu.get_barrier_semaphore()

    @pl.loop(1, n)
    def _(o):
        pl.semaphore_signal(
            barrier, inc=1, device_id={"ep": lax.rem(me + o, n)}, device_id_type=MESH
        )

    staged(0)
    pl.semaphore_wait(barrier, n - 1)

    def spread(src, dst_of_me, send_sem, recv_sem):
        def one(o):
            t = lax.rem(me + o, n)
            return pltpu.make_async_remote_copy(
                src_ref=src,
                dst_ref=dst_of_me,
                send_sem=send_sem.at[o],
                recv_sem=recv_sem.at[me],
                device_id={"ep": t},
                device_id_type=MESH,
            )

        @pl.loop(1, n)
        def _(o):
            one(o).start()

    def drain(src, buffer, send_sem, recv_sem):
        @pl.loop(1, n)
        def _(o):
            s = lax.rem(me + o, n)
            pltpu.make_async_copy(src, buffer.at[s], recv_sem.at[s]).wait()

    def drain_sends(src, buffer, send_sem):
        @pl.loop(1, n)
        def _(o):
            pltpu.make_async_copy(src, buffer.at[0], send_sem.at[o]).wait()

    spread(res_v, gath1.at[me], s1, r1)
    gath1[me] = res_v[...]
    drain(res_v, gath1, s1, r1)
    staged(1)

    def normalise(gath, gain):
        total = jnp.zeros((seqs, own), F32)
        for s in range(n):
            x = gath[s].astype(F32)
            total = total + x * x
        scale = lax.rsqrt(jnp.sum(total, axis=1, keepdims=True) / width + NORM_EPS)
        for s in range(n):
            g = gain[:, s * own : (s + 1) * own].astype(F32)
            lhs[:, s * own : (s + 1) * own] = (gath[s].astype(F32) * scale * g).astype(BF16)

    normalise(gath1, gain1_v)

    def kdot(weights, chunk):
        depth = lhs.shape[1]
        outs = tuple(jnp.zeros((seqs, w.shape[1]), F32) for w in weights)

        def step(i, accs):
            at = pl.ds(pl.multiple_of(i * chunk, chunk), chunk)
            x = lhs[:, at]
            return tuple(
                acc + jnp.dot(x, w[at, :], preferred_element_type=F32)
                for acc, w in zip(accs, weights)
            )

        return lax.fori_loop(0, depth // chunk, step, outs)

    staged(2, 3, 4, 5)
    q, k, v, g = kdot((wq_v, wk_v, wv_v, wg_v), 512)
    row = jnp.concatenate([q, k, v, g], axis=1).astype(BF16).astype(F32)
    for c in range(tiles2):
        part = row[:, c * 128 : (c + 1) * 128]
        for s in range(seqs):
            send2[s, c : c + 1, :] = part[s : s + 1, :]

    my_slot = lax.rem(me, group_src)

    def target2(s):
        return (s * HEADS + src_head) // pairs_dev

    def copy2(s):
        return pltpu.make_async_remote_copy(
            src_ref=send2.at[s],
            dst_ref=recv2.at[my_slot],
            send_sem=s2.at[s],
            recv_sem=r2.at[my_slot],
            device_id={"ep": target2(s)},
            device_id_type=MESH,
        )

    @pl.loop(0, seqs)
    def _(s):
        @pl.when(target2(s) != me)
        def _():
            copy2(s).start()

        @pl.when(target2(s) == me)
        def _():
            pltpu.make_async_copy(send2.at[s], recv2.at[my_slot], r2.at[my_slot]).start()

    staged(6, 7, 8)
    (low,) = kdot((wlow_v,), 1024)
    head_at = pl.ds(pl.multiple_of(my_head0 * DK, DK), pairs_dev * DK)
    pre = jnp.dot(
        low,
        wdec_v[:, head_at].astype(F32),
        preferred_element_type=F32,
        precision=lax.Precision.HIGHEST,
    )
    row_is = lax.broadcasted_iota(jnp.int32, pre.shape, 0) == my_seq
    pre = jnp.sum(jnp.where(row_is, pre, 0.0), axis=0, keepdims=True) + bias_v[:, head_at]
    log_sig = jnp.minimum(pre, 0.0) - jnp.log(1.0 + jnp.exp(-jnp.abs(pre)))
    decay = jnp.exp(log_sig / DECAY_TAU)

    @pl.loop(0, group_src)
    def _(i):
        pltpu.make_async_copy(send2.at[0], recv2.at[i], r2.at[i]).wait()

    def lanes(i, start, size):
        out = []
        while size:
            c, off = start // 128, start % 128
            take = min(size, 128 - off)
            out.append(recv2[i, c : c + 1, :][:, off : off + take])
            start, size = start + take, size - take
        return out

    def gathered_row(p, start, size):
        out = []
        for i in range(dph):
            out.extend(lanes(p * dph + i, start, size))
        return jnp.concatenate(out, axis=1)

    stack = []
    for p in range(pairs_dev):
        stack.append(gathered_row(p, 0, qw) * DK ** (-0.5))
        stack.append(gathered_row(p, qw, qw))
        stack.append(decay[:, p * DK : (p + 1) * DK])
    stack.append(jnp.zeros((8 - len(stack), DK), F32))
    cols[...] = jnp.transpose(jnp.concatenate(stack, axis=0))
    staged(9, 10)
    step_rows = 32
    mixed_rows = []
    for p in range(pairs_dev):
        value = gathered_row(p, 2 * qw, vw)

        def update(i, acc):
            at = pl.ds(pl.multiple_of(i * step_rows, step_rows), step_rows)
            three = cols[at, 3 * p : 3 * p + 3]
            fresh = states_v[p, at, :] * three[:, 2:3] + three[:, 1:2] * value
            states_v[p, at, :] = fresh
            weighted = fresh * three[:, 0:1]
            return acc + jnp.sum(weighted.reshape(step_rows // 8, 8, DV), axis=0)

        acc = lax.fori_loop(0, DK // step_rows, update, jnp.zeros((8, DV), F32))
        pltpu.make_async_copy(states_v.at[p], new_states.at[p], out_sem.at[p]).start()
        read = jnp.sum(acc, axis=0, keepdims=True)
        gate = gathered_row(p, 2 * qw + vw, vw)
        scale = lax.rsqrt(jnp.mean(read * read, axis=1, keepdims=True) + NORM_EPS)
        mixed = read * scale * hgain_v[...].astype(F32) * (gate / (1.0 + jnp.exp(-gate)))
        mixed_rows.extend(mixed[:, c * 128 : (c + 1) * 128] for c in range(DV // 128))
    send3[...] = jnp.concatenate(mixed_rows, axis=0).astype(BF16)

    spread(send3, gath3.at[me], s3, r3)
    gath3[me] = send3[...]
    drain(send3, gath3, s3, r3)
    per_seq = HEADS // pairs_dev
    for d in range(n):
        stage3[d // per_seq, (d % per_seq) * rows3 : (d % per_seq + 1) * rows3, :] = gath3[
            d
        ].astype(F32)
    for c in range(HEADS * DV // 128):
        lhs[:, c * 128 : (c + 1) * 128] = stage3[:, c, :].astype(BF16)
    staged(11)
    (branch,) = kdot((wout_v,), 1024)
    stream = (res_v[...].astype(F32) + branch.astype(BF16).astype(F32)).astype(BF16)
    stream_v[...] = stream

    spread(stream_v, gath4.at[me], s4, r4)
    gath4[me] = stream
    staged(12, 13, 14, 15)
    group_exp = jnp.exp(glog_v[...])
    group_prob = group_exp / jnp.sum(group_exp, axis=1, keepdims=True)
    route = routes_v[...]
    chosen = route[:, 0:1] // (n // GROUPS)
    group_is = lax.broadcasted_iota(jnp.int32, group_prob.shape, 1) == chosen
    picked = jnp.sum(jnp.where(group_is, group_prob, 0.0), axis=1, keepdims=True)
    expert_exp = jnp.exp(elog_v[...])
    weights = expert_exp / jnp.sum(expert_exp, axis=1, keepdims=True) * picked
    mine = jnp.sum(jnp.where(route == me, weights, 0.0), axis=1, keepdims=True)
    drain(stream_v, gath4, s4, r4)
    normalise(gath4, gain2_v)
    staged(16, 17)
    gate_part, up_part = kdot((eg_v.at[0], eu_v.at[0]), 512)
    active = (gate_part / (1.0 + jnp.exp(-gate_part)) * up_part * mine).astype(BF16)
    staged(18)

    def copy5(o):
        t = lax.rem(me + o, n)
        return pltpu.make_async_remote_copy(
            src_ref=send5.at[o],
            dst_ref=recv5.at[me],
            send_sem=s5.at[o],
            recv_sem=r5.at[me],
            device_id={"ep": t},
            device_id_type=MESH,
        )

    def contribution(t):
        at = pl.ds(pl.multiple_of(t * own, own), own)
        return jnp.dot(active, ed_v[0, :, at], preferred_element_type=F32).astype(BF16)

    @pl.loop(1, n)
    def _(o):
        send5[o] = contribution(lax.rem(me + o, n))
        copy5(o).start()

    recv5[me] = contribution(me)
    drain(stream_v, recv5, s5, r5)
    total = jnp.zeros((seqs, own), F32)
    for s in range(n):
        total = total + recv5[s].astype(F32)
    out_v[...] = (stream.astype(F32) + total).astype(BF16)
    out_copy = pltpu.make_async_copy(out_v, layer_out, out_sem.at[pairs_dev])
    out_copy.start()

    drain_sends(res_v, gath1, s1)
    drain_sends(send3, gath3, s3)
    drain_sends(stream_v, gath4, s4)
    drain_sends(stream_v, recv5, s5)

    @pl.loop(0, seqs)
    def _(s):
        @pl.when(target2(s) != me)
        def _():
            copy2(s).wait_send()

    for p in range(pairs_dev):
        pltpu.make_async_copy(states_v.at[p], new_states.at[p], out_sem.at[p]).wait()
    out_copy.wait()


def per_device(*args):
    n = lax.axis_size("ep")
    args = list(args)
    for i in (2, 9, 10, 12):
        args[i] = args[i].reshape(1, -1)
    residual, head_states = args[0], args[1]
    seqs, own = residual.shape
    pairs_dev = head_states.shape[0]
    width = own * n
    qw, vw = args[3].shape[1], args[5].shape[1]
    group_src = pairs_dev * (n // HEADS)
    tiles2 = (2 * qw + 2 * vw) // 128
    rows3 = pairs_dev * DV // 128
    dma = pltpu.SemaphoreType.DMA
    stage = [pltpu.VMEM(a.shape, a.dtype) for a in args]
    return pl.pallas_call(
        functools.partial(kernel_body, n),
        out_shape=(
            jax.ShapeDtypeStruct(residual.shape, BF16),
            jax.ShapeDtypeStruct(head_states.shape, F32),
        ),
        in_specs=[pl.BlockSpec(memory_space=pl.ANY)] * len(args),
        out_specs=(pl.BlockSpec(memory_space=pl.ANY),) * 2,
        scratch_shapes=stage
        + [
            pltpu.VMEM((n, seqs, own), BF16),
            pltpu.VMEM((seqs, width), BF16),
            pltpu.VMEM((seqs, tiles2, 128), F32),
            pltpu.VMEM((group_src, tiles2, 128), F32),
            pltpu.VMEM((DK, 8), F32),
            pltpu.VMEM((rows3, 128), BF16),
            pltpu.VMEM((n, rows3, 128), BF16),
            pltpu.VMEM((seqs, HEADS * DV // 128, 128), F32),
            pltpu.VMEM((seqs, own), BF16),
            pltpu.VMEM((n, seqs, own), BF16),
            pltpu.VMEM((n, seqs, own), BF16),
            pltpu.VMEM((n, seqs, own), BF16),
            pltpu.VMEM((seqs, own), BF16),
            dma((len(args),)),
            dma((pairs_dev + 1,)),
            dma((n,)),
            dma((n,)),
            dma((seqs,)),
            dma((group_src,)),
            dma((n,)),
            dma((n,)),
            dma((n,)),
            dma((n,)),
            dma((n,)),
            dma((n,)),
        ],
        compiler_params=pltpu.CompilerParams(
            collective_id=0, has_side_effects=True, vmem_limit_bytes=56 * 1024 * 1024
        ),
        name="layer",
    )(*args)


def solution(mesh):
    return jax.shard_map(
        per_device,
        mesh=mesh,
        in_specs=(
            P("grp", "ep"),
            P(("grp", "ep"), None, None),
            P(),
            P(None, "ep"),
            P(None, "ep"),
            P(None, "ep"),
            P(None, "ep"),
            P(),
            P(),
            P(),
            P(),
            P(None, "ep"),
            P(),
            P("grp", None),
            P("grp", None),
            P("grp", None),
            P("ep", None, None),
            P("ep", None, None),
            P("ep", None, None),
        ),
        out_specs=(P("grp", "ep"), P(("grp", "ep"), None, None)),
        check_vma=False,
    )
```

```python
import functools

import jax
import jax.numpy as jnp
from jax import lax
from jax.experimental import pallas as pl
from jax.experimental.pallas import tpu as pltpu
from jax.sharding import PartitionSpec as P

HEADS = 4
DK = 512
DV = 1024
GROUPS = 4

NORM_EPS = 1e-06
DECAY_TAU = 16.0
MESH = pl.DeviceIdType.MESH
F32 = jnp.float32
BF16 = jnp.bfloat16


def kernel_body(n, *refs):
    (
        residual,
        head_states,
        first_gain,
        w_query,
        w_key,
        w_value,
        w_gate,
        w_low,
        w_decay,
        decay_bias,
        head_gain,
        w_output,
        second_gain,
        routes,
        group_logits,
        expert_logits,
        expert_gate,
        expert_up,
        expert_down,
        layer_out,
        new_states,
        res_v,
        gain1_v,
        wq_v,
        wk_v,
        wv_v,
        wg_v,
        wlow_v,
        wdec_v,
        bias_v,
        hgain_v,
        wout_v,
        gain2_v,
        routes_v,
        glog_v,
        elog_v,
        eg_v,
        eu_v,
        ed_v,
        gath1,
        lhs,
        send2,
        recv2,
        cols,
        send3,
        gath3,
        stage3,
        stream_v,
        gath4,
        send5,
        recv5,
        local_sem,
        s1,
        r1,
        s2,
        r2,
        s3,
        r3,
        s4,
        r4,
        s5,
        r5,
    ) = refs
    states_v = new_states
    me = lax.axis_index("ep")
    seqs, own = residual.shape
    width = own * n
    pairs_dev = head_states.shape[0]
    dph = n // HEADS
    qw, vw = w_query.shape[1], w_value.shape[1]
    group_src = pairs_dev * dph
    my_seq = me * pairs_dev // HEADS
    my_head0 = lax.rem(me * pairs_dev, HEADS)
    src_head = me // dph
    tiles2 = send2.shape[1]
    rows3 = send3.shape[0]

    pieces = [
        (residual, res_v),
        (first_gain, gain1_v),
        (w_query, wq_v),
        (w_key, wk_v),
        (w_value, wv_v),
        (w_gate, wg_v),
        (w_low, wlow_v),
        (w_decay, wdec_v),
        (decay_bias, bias_v),
        (head_states, states_v),
        (head_gain, hgain_v),
        (w_output, wout_v),
        (second_gain, gain2_v),
        (routes, routes_v),
        (group_logits, glog_v),
        (expert_logits, elog_v),
        (expert_gate, eg_v),
        (expert_up, eu_v),
        (expert_down, ed_v),
    ]
    copies = [
        pltpu.make_async_copy(src, dst, local_sem.at[i]) for i, (src, dst) in enumerate(pieces)
    ]
    for copy in copies:
        copy.start()

    def staged(*indices):
        for i in indices:
            copies[i].wait()

    barrier = pltpu.get_barrier_semaphore()

    @pl.loop(1, n)
    def _(o):
        pl.semaphore_signal(
            barrier, inc=1, device_id={"ep": lax.rem(me + o, n)}, device_id_type=MESH
        )

    staged(0)
    pl.semaphore_wait(barrier, n - 1)

    def spread(src, dst_of_me, send_sem, recv_sem):
        def one(o):
            t = lax.rem(me + o, n)
            return pltpu.make_async_remote_copy(
                src_ref=src,
                dst_ref=dst_of_me,
                send_sem=send_sem.at[o],
                recv_sem=recv_sem.at[me],
                device_id={"ep": t},
                device_id_type=MESH,
            )

        @pl.loop(1, n)
        def _(o):
            one(o).start()

    def drain(src, buffer, send_sem, recv_sem):
        @pl.loop(1, n)
        def _(o):
            s = lax.rem(me + o, n)
            pltpu.make_async_copy(src, buffer.at[s], recv_sem.at[s]).wait()

    def drain_sends(src, buffer, send_sem):
        @pl.loop(1, n)
        def _(o):
            pltpu.make_async_copy(src, buffer.at[0], send_sem.at[o]).wait()

    spread(res_v, gath1.at[me], s1, r1)
    gath1[me] = res_v[...]
    drain(res_v, gath1, s1, r1)
    staged(1)

    def normalise(gath, gain):
        total = jnp.zeros((seqs, own), F32)
        for s in range(n):
            x = gath[s].astype(F32)
            total = total + x * x
        scale = lax.rsqrt(jnp.sum(total, axis=1, keepdims=True) / width + NORM_EPS)
        gains = gain[...].astype(F32)
        per = own // 128
        for s in range(n):
            g = jnp.concatenate(
                [gains[s * per + c : s * per + c + 1, :] for c in range(per)], axis=1
            )
            lhs[:, s * own : (s + 1) * own] = (gath[s].astype(F32) * scale * g).astype(BF16)

    normalise(gath1, gain1_v)

    def kdot(weights, chunk):
        depth = lhs.shape[1]
        outs = tuple(jnp.zeros((seqs, w.shape[1]), F32) for w in weights)

        def step(i, accs):
            at = pl.ds(pl.multiple_of(i * chunk, chunk), chunk)
            x = lhs[:, at]
            return tuple(
                acc + jnp.dot(x, w[at, :], preferred_element_type=F32)
                for acc, w in zip(accs, weights)
            )

        return lax.fori_loop(0, depth // chunk, step, outs)

    staged(2, 3, 4, 5)
    q, k, v, g = kdot((wq_v, wk_v, wv_v, wg_v), 512)
    row = jnp.concatenate([q, k, v, g], axis=1).astype(BF16).astype(F32)
    for c in range(tiles2):
        part = row[:, c * 128 : (c + 1) * 128]
        for s in range(seqs):
            send2[s, c : c + 1, :] = part[s : s + 1, :]

    my_slot = lax.rem(me, group_src)

    def target2(s):
        return (s * HEADS + src_head) // pairs_dev

    def copy2(s):
        return pltpu.make_async_remote_copy(
            src_ref=send2.at[s],
            dst_ref=recv2.at[my_slot],
            send_sem=s2.at[s],
            recv_sem=r2.at[my_slot],
            device_id={"ep": target2(s)},
            device_id_type=MESH,
        )

    @pl.loop(0, seqs)
    def _(s):
        @pl.when(target2(s) != me)
        def _():
            copy2(s).start()

        @pl.when(target2(s) == me)
        def _():
            pltpu.make_async_copy(send2.at[s], recv2.at[my_slot], r2.at[my_slot]).start()

    staged(6, 7, 8)
    low = lax.dot_general(
        lhs[...], wlow_v[...], (((1,), (1,)), ((), ())), preferred_element_type=F32
    )
    head_at = pl.ds(pl.multiple_of(my_head0 * DK, DK), pairs_dev * DK)
    pre = jnp.dot(
        low,
        wdec_v[:, head_at].astype(F32),
        preferred_element_type=F32,
        precision=lax.Precision.HIGHEST,
    )
    row_is = lax.broadcasted_iota(jnp.int32, pre.shape, 0) == my_seq
    pre = jnp.sum(jnp.where(row_is, pre, 0.0), axis=0, keepdims=True) + bias_v[:, head_at]
    log_sig = jnp.minimum(pre, 0.0) - jnp.log(1.0 + jnp.exp(-jnp.abs(pre)))
    decay = jnp.exp(log_sig / DECAY_TAU)

    @pl.loop(0, group_src)
    def _(i):
        pltpu.make_async_copy(send2.at[0], recv2.at[i], r2.at[i]).wait()

    def lanes(i, start, size):
        out = []
        while size:
            c, off = start // 128, start % 128
            take = min(size, 128 - off)
            out.append(recv2[i, c : c + 1, :][:, off : off + take])
            start, size = start + take, size - take
        return out

    def gathered_row(p, start, size):
        out = []
        for i in range(dph):
            out.extend(lanes(p * dph + i, start, size))
        return jnp.concatenate(out, axis=1)

    def folded(row):
        return jnp.concatenate(
            [row[:, c * 128 : (c + 1) * 128] for c in range(row.shape[1] // 128)], axis=0
        )

    stack = []
    for p in range(pairs_dev):
        stack.append(gathered_row(p, 0, qw) * DK ** (-0.5))
        stack.append(gathered_row(p, qw, qw))
        stack.append(decay[:, p * DK : (p + 1) * DK])
    stack.append(jnp.zeros((8 - len(stack), DK), F32))
    cols[...] = jnp.transpose(jnp.concatenate(stack, axis=0))
    staged(9, 10)
    step_rows = 32
    mixed_rows = []
    for p in range(pairs_dev):
        value = gathered_row(p, 2 * qw, vw)

        def update(i, acc):
            at = pl.ds(pl.multiple_of(i * step_rows, step_rows), step_rows)
            three = cols[at, 3 * p : 3 * p + 3]
            fresh = states_v[p, at, :] * three[:, 2:3] + three[:, 1:2] * value
            states_v[p, at, :] = fresh
            weighted = fresh * three[:, 0:1]
            return acc + jnp.sum(weighted.reshape(step_rows // 8, 8, DV), axis=0)

        acc = lax.fori_loop(0, DK // step_rows, update, jnp.zeros((8, DV), F32))
        read = jnp.sum(acc, axis=0, keepdims=True)
        scale = lax.rsqrt(jnp.mean(read * read, axis=1, keepdims=True) + NORM_EPS)
        read = folded(read)
        gate = folded(gathered_row(p, 2 * qw + vw, vw))
        mixed = read * scale * hgain_v[...].astype(F32) * (gate / (1.0 + jnp.exp(-gate)))
        mixed_rows.append(mixed)
    send3[...] = jnp.concatenate(mixed_rows, axis=0).astype(BF16)

    spread(send3, gath3.at[me], s3, r3)
    gath3[me] = send3[...]
    drain(send3, gath3, s3, r3)
    per_seq = HEADS // pairs_dev
    for d in range(n):
        stage3[d // per_seq, (d % per_seq) * rows3 : (d % per_seq + 1) * rows3, :] = gath3[
            d
        ].astype(F32)
    for c in range(HEADS * DV // 128):
        lhs[:, c * 128 : (c + 1) * 128] = stage3[:, c, :].astype(BF16)
    staged(11)
    (branch,) = kdot((wout_v,), 1024)
    stream = (res_v[...].astype(F32) + branch.astype(BF16).astype(F32)).astype(BF16)
    stream_v[...] = stream

    spread(stream_v, gath4.at[me], s4, r4)
    gath4[me] = stream
    staged(12, 13, 14, 15)
    group_exp = jnp.exp(glog_v[...])
    group_prob = group_exp / jnp.sum(group_exp, axis=0, keepdims=True)
    route = routes_v[...]
    chosen = route[0:1, :] // (n // GROUPS)
    group_is = lax.broadcasted_iota(jnp.int32, group_prob.shape, 0) == chosen
    picked = jnp.sum(jnp.where(group_is, group_prob, 0.0), axis=0, keepdims=True)
    expert_exp = jnp.exp(elog_v[...])
    weights = expert_exp / jnp.sum(expert_exp, axis=0, keepdims=True) * picked
    mine = jnp.sum(jnp.where(route == me, weights, 0.0), axis=0, keepdims=True)
    diagonal = lax.broadcasted_iota(jnp.int32, (seqs, seqs), 0) == lax.broadcasted_iota(
        jnp.int32, (seqs, seqs), 1
    )
    mine = jnp.sum(jnp.where(diagonal, mine, 0.0), axis=1, keepdims=True)
    drain(stream_v, gath4, s4, r4)
    normalise(gath4, gain2_v)
    staged(16, 17)
    gate_part, up_part = kdot((eg_v.at[0], eu_v.at[0]), 512)
    active = (gate_part / (1.0 + jnp.exp(-gate_part)) * up_part * mine).astype(BF16)
    staged(18)

    def copy5(o):
        t = lax.rem(me + o, n)
        return pltpu.make_async_remote_copy(
            src_ref=send5.at[o],
            dst_ref=recv5.at[me],
            send_sem=s5.at[o],
            recv_sem=r5.at[me],
            device_id={"ep": t},
            device_id_type=MESH,
        )

    def contribution(t):
        at = pl.ds(pl.multiple_of(t * own, own), own)
        return jnp.dot(active, ed_v[0, :, at], preferred_element_type=F32).astype(BF16)

    @pl.loop(1, n)
    def _(o):
        send5[o] = contribution(lax.rem(me + o, n))
        copy5(o).start()

    recv5[me] = contribution(me)
    drain(stream_v, recv5, s5, r5)
    total = jnp.zeros((seqs, own), F32)
    for s in range(n):
        total = total + recv5[s].astype(F32)
    layer_out[...] = (stream.astype(F32) + total).astype(BF16)

    drain_sends(res_v, gath1, s1)
    drain_sends(send3, gath3, s3)
    drain_sends(stream_v, gath4, s4)
    drain_sends(stream_v, recv5, s5)

    @pl.loop(0, seqs)
    def _(s):
        @pl.when(target2(s) != me)
        def _():
            copy2(s).wait_send()


def per_device(*args):
    n = lax.axis_size("ep")
    args = list(args)
    for i in (2, 10, 12):
        args[i] = args[i].reshape(-1, 128)
    args[9] = args[9].reshape(1, -1)
    for i in (7, 13, 14, 15):
        args[i] = args[i].T
    args = [pltpu.with_memory_space_constraint(a, pltpu.HBM) for a in args]
    residual, head_states = args[0], args[1]
    seqs, own = residual.shape
    pairs_dev = head_states.shape[0]
    width = own * n
    qw, vw = args[3].shape[1], args[5].shape[1]
    group_src = pairs_dev * (n // HEADS)
    tiles2 = (2 * qw + 2 * vw) // 128
    rows3 = pairs_dev * DV // 128
    dma = pltpu.SemaphoreType.DMA
    stage = [pltpu.VMEM(a.shape, a.dtype) for i, a in enumerate(args) if i != 1]
    return pl.pallas_call(
        functools.partial(kernel_body, n),
        out_shape=(
            pltpu.VMEM(residual.shape, BF16),
            pltpu.VMEM(head_states.shape, F32),
        ),
        in_specs=[pl.BlockSpec(memory_space=pltpu.HBM)] * len(args),
        out_specs=(pl.BlockSpec(memory_space=pltpu.VMEM),) * 2,
        scratch_shapes=stage
        + [
            pltpu.VMEM((n, seqs, own), BF16),
            pltpu.VMEM((seqs, width), BF16),
            pltpu.VMEM((seqs, tiles2, 128), F32),
            pltpu.VMEM((group_src, tiles2, 128), F32),
            pltpu.VMEM((DK, 8), F32),
            pltpu.VMEM((rows3, 128), BF16),
            pltpu.VMEM((n, rows3, 128), BF16),
            pltpu.VMEM((seqs, HEADS * DV // 128, 128), F32),
            pltpu.VMEM((seqs, own), BF16),
            pltpu.VMEM((n, seqs, own), BF16),
            pltpu.VMEM((n, seqs, own), BF16),
            pltpu.VMEM((n, seqs, own), BF16),
            dma((len(args),)),
            dma((n,)),
            dma((n,)),
            dma((seqs,)),
            dma((group_src,)),
            dma((n,)),
            dma((n,)),
            dma((n,)),
            dma((n,)),
            dma((n,)),
            dma((n,)),
        ],
        compiler_params=pltpu.CompilerParams(
            collective_id=0, has_side_effects=True, vmem_limit_bytes=48 * 1024 * 1024
        ),
        name="layer",
    )(*args)


def solution(mesh):
    return jax.shard_map(
        per_device,
        mesh=mesh,
        in_specs=(
            P("grp", "ep"),
            P(("grp", "ep"), None, None),
            P(),
            P(None, "ep"),
            P(None, "ep"),
            P(None, "ep"),
            P(None, "ep"),
            P(),
            P(),
            P(),
            P(),
            P(None, "ep"),
            P(),
            P("grp", None),
            P("grp", None),
            P("grp", None),
            P("ep", None, None),
            P("ep", None, None),
            P("ep", None, None),
        ),
        out_specs=(P("grp", "ep"), P(("grp", "ep"), None, None)),
        check_vma=False,
    )
```

```python
import functools

import jax
import jax.numpy as jnp
from jax import lax
from jax.experimental import pallas as pl
from jax.experimental.pallas import tpu as pltpu
from jax.sharding import PartitionSpec as P

HEADS = 4
DK = 512
DV = 1024
GROUPS = 4

NORM_EPS = 1e-06
DECAY_TAU = 16.0
MESH = pl.DeviceIdType.MESH
F32 = jnp.float32
BF16 = jnp.bfloat16


def kernel_body(n, *refs):
    (
        residual,
        head_states,
        first_gain,
        w_query,
        w_key,
        w_value,
        w_gate,
        w_low,
        w_decay,
        decay_bias,
        head_gain,
        w_output,
        second_gain,
        routes,
        group_logits,
        expert_logits,
        expert_gate,
        expert_up,
        expert_down,
        layer_out,
        new_states,
        res_v,
        gain1_v,
        wq_v,
        wk_v,
        wv_v,
        wg_v,
        wlow_v,
        wdec_v,
        bias_v,
        hgain_v,
        wout_v,
        gain2_v,
        routes_v,
        glog_v,
        elog_v,
        eg_v,
        eu_v,
        ed_v,
        gath1,
        lhs,
        send2,
        recv2,
        cols,
        send3,
        gath3,
        stage3,
        gain1_f,
        gain2_f,
        stream_v,
        gath4,
        send5,
        recv5,
        local_sem,
        s1,
        r1,
        s2,
        r2,
        s3,
        r3,
        s4,
        r4,
        s5,
        r5,
    ) = refs
    states_v = new_states
    me = lax.axis_index("ep")
    seqs, own = residual.shape
    width = own * n
    pairs_dev = head_states.shape[0]
    dph = n // HEADS
    qw, vw = w_query.shape[1], w_value.shape[1]
    group_src = pairs_dev * dph
    my_seq = me * pairs_dev // HEADS
    my_head0 = lax.rem(me * pairs_dev, HEADS)
    src_head = me // dph
    tiles2 = send2.shape[1]
    rows3 = send3.shape[0]

    pieces = [
        (residual, res_v),
        (first_gain, gain1_v),
        (w_query, wq_v),
        (w_key, wk_v),
        (w_value, wv_v),
        (w_gate, wg_v),
        (w_low, wlow_v),
        (w_decay, wdec_v),
        (decay_bias, bias_v),
        (head_states, states_v),
        (head_gain, hgain_v),
        (w_output, wout_v),
        (second_gain, gain2_v),
        (routes, routes_v),
        (group_logits, glog_v),
        (expert_logits, elog_v),
        (expert_gate, eg_v),
        (expert_up, eu_v),
        (expert_down, ed_v),
    ]
    copies = [
        pltpu.make_async_copy(src, dst, local_sem.at[i]) for i, (src, dst) in enumerate(pieces)
    ]
    for copy in copies:
        copy.start()

    def staged(*indices):
        for i in indices:
            copies[i].wait()

    barrier = pltpu.get_barrier_semaphore()

    @pl.loop(1, n)
    def _(o):
        pl.semaphore_signal(
            barrier, inc=1, device_id={"ep": lax.rem(me + o, n)}, device_id_type=MESH
        )

    staged(0)
    pl.semaphore_wait(barrier, n - 1)

    bit_count = n.bit_length() - 1
    signs = [1 - 2 * lax.rem(me // 2**b, 2) for b in range(bit_count)]

    def partner_of(o):
        if 2**bit_count != n:
            return lax.rem(me + o, n)
        return me + sum(signs[b] * 2**b for b in range(bit_count) if o >> b & 1)

    partner = [partner_of(o) for o in range(n)]
    far_first = range(n - 1, 0, -1)

    def send(src, dst, send_sem, recv_sem, target):
        pltpu.make_async_remote_copy(
            src_ref=src,
            dst_ref=dst,
            send_sem=send_sem,
            recv_sem=recv_sem,
            device_id={"ep": target},
            device_id_type=MESH,
        ).start()

    def wait_blocks(buffer, sem):
        part = buffer.at[pl.ds(0, n - 1)]
        pltpu.make_async_copy(part, part, sem).wait()

    per = own // 128
    own_at = [pl.ds(pl.multiple_of(t * own, own), own) for t in partner]

    def absorb(gath, recv_sem, gains, weights, keep):
        accs = [jnp.zeros((seqs, w.shape[-1]), F32) for w in weights]
        total = jnp.zeros((seqs, own), F32)
        for o in range(n):
            t = partner[o]
            if o:
                block = gath.at[t]
                pltpu.make_async_copy(block, block, recv_sem.at[t]).wait()
            x = gath[t].astype(F32)
            total = total + x * x
            gain = jnp.concatenate([gains[pl.ds(t * per + c, 1), :] for c in range(per)], axis=1)
            x = (x * gain).astype(BF16)
            if keep:
                lhs[:, own_at[o]] = x
            accs = [
                acc + jnp.dot(x, w[own_at[o], :], preferred_element_type=F32)
                for acc, w in zip(accs, weights)
            ]
        scale = lax.rsqrt(jnp.sum(total, axis=1, keepdims=True) / width + NORM_EPS)
        return scale, [acc * scale for acc in accs]

    for o in far_first:
        send(res_v, gath1.at[me], s1.at[0], r1.at[me], partner[o])
    gath1[me] = res_v[...]
    staged(1)
    gain1_f[...] = gain1_v[...].astype(F32)
    staged(2, 3, 4, 5)
    scale1, (q, k, v, g) = absorb(gath1, r1, gain1_f, (wq_v, wk_v, wv_v, wg_v), True)
    row = jnp.concatenate([q, k, v, g], axis=1).astype(BF16).astype(F32)
    for c in range(tiles2):
        part = row[:, c * 128 : (c + 1) * 128]
        for s in range(seqs):
            send2[s, c : c + 1, :] = part[s : s + 1, :]

    my_slot = lax.rem(me, group_src)

    def target2(s):
        return (s * HEADS + src_head) // pairs_dev

    def copy2(s):
        return pltpu.make_async_remote_copy(
            src_ref=send2.at[s],
            dst_ref=recv2.at[my_slot],
            send_sem=s2.at[s],
            recv_sem=r2.at[my_slot],
            device_id={"ep": target2(s)},
            device_id_type=MESH,
        )

    @pl.loop(0, seqs)
    def _(s):
        @pl.when(target2(s) != me)
        def _():
            copy2(s).start()

        @pl.when(target2(s) == me)
        def _():
            pltpu.make_async_copy(send2.at[s], recv2.at[my_slot], r2.at[my_slot]).start()

    staged(6, 7, 8)
    low = scale1 * lax.dot_general(
        lhs[...], wlow_v[...], (((1,), (1,)), ((), ())), preferred_element_type=F32
    )
    head_at = pl.ds(pl.multiple_of(my_head0 * DK, DK), pairs_dev * DK)
    pre = jnp.dot(
        low,
        wdec_v[:, head_at].astype(F32),
        preferred_element_type=F32,
        precision=lax.Precision.HIGHEST,
    )
    row_is = lax.broadcasted_iota(jnp.int32, pre.shape, 0) == my_seq
    pre = jnp.sum(jnp.where(row_is, pre, 0.0), axis=0, keepdims=True) + bias_v[:, head_at]
    log_sig = jnp.minimum(pre, 0.0) - jnp.log(1.0 + jnp.exp(-jnp.abs(pre)))
    decay = jnp.exp(log_sig / DECAY_TAU)

    @pl.loop(0, group_src)
    def _(i):
        pltpu.make_async_copy(send2.at[0], recv2.at[i], r2.at[i]).wait()

    def lanes(i, start, size):
        out = []
        while size:
            c, off = start // 128, start % 128
            take = min(size, 128 - off)
            out.append(recv2[i, c : c + 1, :][:, off : off + take])
            start, size = start + take, size - take
        return out

    def gathered_row(p, start, size):
        out = []
        for i in range(dph):
            out.extend(lanes(p * dph + i, start, size))
        return jnp.concatenate(out, axis=1)

    def folded(row):
        return jnp.concatenate(
            [row[:, c * 128 : (c + 1) * 128] for c in range(row.shape[1] // 128)], axis=0
        )

    stack, overlap = [], []
    for p in range(pairs_dev):
        query = gathered_row(p, 0, qw) * DK ** (-0.5)
        key = gathered_row(p, qw, qw)
        fade = decay[:, p * DK : (p + 1) * DK]
        stack.extend([query * fade, key, fade])
        overlap.append(jnp.sum(query * key, axis=1, keepdims=True))
    stack.append(jnp.zeros((8 - len(stack), DK), F32))
    cols[...] = jnp.transpose(jnp.concatenate(stack, axis=0))
    values = [gathered_row(p, 2 * qw, vw) for p in range(pairs_dev)]
    staged(9, 10)
    step_rows = 128

    def read_step(i, accs):
        base = pl.multiple_of(i * step_rows, step_rows)
        out = []
        for p, acc in enumerate(accs):
            fading = cols[pl.ds(base, step_rows), 3 * p : 3 * p + 1]
            for r in range(0, step_rows, 8):
                acc = acc + states_v[p, pl.ds(base + r, 8), :] * fading[r : r + 8]
            out.append(acc)
        return tuple(out)

    zero = jnp.zeros((8, DV), F32)
    accs = lax.fori_loop(0, DK // step_rows, read_step, (zero,) * pairs_dev)
    mixed_rows = []
    for p in range(pairs_dev):
        read = jnp.sum(accs[p], axis=0, keepdims=True) + overlap[p] * values[p]
        scale = lax.rsqrt(jnp.mean(read * read, axis=1, keepdims=True) + NORM_EPS)
        read = folded(read)
        gate = folded(gathered_row(p, 2 * qw + vw, vw))
        mixed = read * scale * hgain_v[...].astype(F32) * (gate / (1.0 + jnp.exp(-gate)))
        mixed_rows.append(mixed)
    send3[...] = jnp.concatenate(mixed_rows, axis=0).astype(BF16)

    for o in far_first:
        send(send3, gath3.at[me], s3.at[0], r3.at[0], partner[o])
    gath3[me] = send3[...]

    @pl.loop(0, DK // step_rows)
    def _(i):
        base = pl.multiple_of(i * step_rows, step_rows)
        for p in range(pairs_dev):
            keys = cols[pl.ds(base, step_rows), 3 * p + 1 : 3 * p + 2]
            fades = cols[pl.ds(base, step_rows), 3 * p + 2 : 3 * p + 3]
            for r in range(0, step_rows, 8):
                at = pl.ds(base + r, 8)
                states_v[p, at, :] = (
                    states_v[p, at, :] * fades[r : r + 8] + keys[r : r + 8] * values[p]
                )

    staged(12, 13, 14, 15)
    gain2_f[...] = gain2_v[...].astype(F32)
    group_exp = jnp.exp(glog_v[...])
    group_prob = group_exp / jnp.sum(group_exp, axis=0, keepdims=True)
    route = routes_v[...]
    chosen = route[0:1, :] // (n // GROUPS)
    group_is = lax.broadcasted_iota(jnp.int32, group_prob.shape, 0) == chosen
    picked = jnp.sum(jnp.where(group_is, group_prob, 0.0), axis=0, keepdims=True)
    expert_exp = jnp.exp(elog_v[...])
    weights = expert_exp / jnp.sum(expert_exp, axis=0, keepdims=True) * picked
    mine = jnp.sum(jnp.where(route == me, weights, 0.0), axis=0, keepdims=True)
    diagonal = lax.broadcasted_iota(jnp.int32, (seqs, seqs), 0) == lax.broadcasted_iota(
        jnp.int32, (seqs, seqs), 1
    )
    mine = jnp.sum(jnp.where(diagonal, mine, 0.0), axis=1, keepdims=True)
    others3 = gath3.at[pl.ds(0, n - 1)]
    pltpu.make_async_copy(others3, others3, r3.at[0]).wait()
    per_seq = HEADS // pairs_dev
    for d in range(n):
        stage3[d // per_seq, (d % per_seq) * rows3 : (d % per_seq + 1) * rows3, :] = gath3[
            d
        ].astype(F32)
    for c in range(HEADS * DV // 128):
        lhs[:, c * 128 : (c + 1) * 128] = stage3[:, c, :].astype(BF16)
    staged(11)
    branch = jnp.dot(lhs[...], wout_v[...], preferred_element_type=F32)
    stream = (res_v[...].astype(F32) + branch.astype(BF16).astype(F32)).astype(BF16)
    stream_v[...] = stream

    for o in far_first:
        send(stream_v, gath4.at[me], s4.at[0], r4.at[me], partner[o])
    gath4[me] = stream
    staged(16, 17, 18)
    _, (gate_part, up_part) = absorb(gath4, r4, gain2_f, (eg_v.at[0], eu_v.at[0]), False)
    active = (gate_part / (1.0 + jnp.exp(-gate_part)) * up_part * mine).astype(BF16)

    def contribution(o):
        return jnp.dot(active, ed_v[0, :, own_at[o]], preferred_element_type=F32).astype(BF16)

    group = 4
    for first in range(n - 1, 0, -group):
        some = range(first, max(first - group, 0), -1)
        for o in some:
            send5[o] = contribution(o)
        for o in some:
            send(send5.at[o], recv5.at[me], s5.at[0], r5.at[0], partner[o])
    recv5[me] = contribution(0)
    wait_blocks(recv5, r5.at[0])
    total = jnp.zeros((seqs, own), F32)
    for s in range(n):
        total = total + recv5[s].astype(F32)
    layer_out[...] = (stream.astype(F32) + total).astype(BF16)

    wait_blocks(gath1, s1.at[0])
    wait_blocks(gath3, s3.at[0])
    wait_blocks(gath4, s4.at[0])
    wait_blocks(recv5, s5.at[0])

    @pl.loop(0, seqs)
    def _(s):
        @pl.when(target2(s) != me)
        def _():
            copy2(s).wait_send()


PUTS = 4


def put_body(layer_out, new_states, layer_hbm, states_hbm, sem):
    copies = [pltpu.make_async_copy(layer_out, layer_hbm, sem.at[0])]
    rows = DK // PUTS
    for p in range(new_states.shape[0]):
        for i in range(PUTS):
            at = pl.ds(i * rows, rows)
            copies.append(
                pltpu.make_async_copy(
                    new_states.at[p, at], states_hbm.at[p, at], sem.at[len(copies)]
                )
            )
    for copy in copies:
        copy.start()
    for copy in copies:
        copy.wait()


def per_device(*args):
    n = lax.axis_size("ep")
    args = list(args)
    for i in (2, 10, 12):
        args[i] = args[i].reshape(-1, 128)
    args[9] = args[9].reshape(1, -1)
    for i in (7, 13, 14, 15):
        args[i] = args[i].T
    args = [pltpu.with_memory_space_constraint(a, pltpu.HBM) for a in args]
    residual, head_states = args[0], args[1]
    seqs, own = residual.shape
    pairs_dev = head_states.shape[0]
    width = own * n
    qw, vw = args[3].shape[1], args[5].shape[1]
    group_src = pairs_dev * (n // HEADS)
    tiles2 = (2 * qw + 2 * vw) // 128
    rows3 = pairs_dev * DV // 128
    dma = pltpu.SemaphoreType.DMA
    stage = [pltpu.VMEM(a.shape, a.dtype) for i, a in enumerate(args) if i != 1]
    results = pl.pallas_call(
        functools.partial(kernel_body, n),
        out_shape=(
            pltpu.VMEM(residual.shape, BF16),
            pltpu.VMEM(head_states.shape, F32),
        ),
        in_specs=[pl.BlockSpec(memory_space=pltpu.HBM)] * len(args),
        out_specs=(pl.BlockSpec(memory_space=pltpu.VMEM),) * 2,
        scratch_shapes=stage
        + [
            pltpu.VMEM((n, seqs, own), BF16),
            pltpu.VMEM((seqs, width), BF16),
            pltpu.VMEM((seqs, tiles2, 128), F32),
            pltpu.VMEM((group_src, tiles2, 128), F32),
            pltpu.VMEM((DK, 8), F32),
            pltpu.VMEM((rows3, 128), BF16),
            pltpu.VMEM((n, rows3, 128), BF16),
            pltpu.VMEM((seqs, HEADS * DV // 128, 128), F32),
            pltpu.VMEM((width // 128, 128), F32),
            pltpu.VMEM((width // 128, 128), F32),
            pltpu.VMEM((seqs, own), BF16),
            pltpu.VMEM((n, seqs, own), BF16),
            pltpu.VMEM((n, seqs, own), BF16),
            pltpu.VMEM((n, seqs, own), BF16),
            dma((len(args),)),
            dma((1,)),
            dma((n,)),
            dma((seqs,)),
            dma((group_src,)),
            dma((1,)),
            dma((1,)),
            dma((1,)),
            dma((n,)),
            dma((1,)),
            dma((1,)),
        ],
        compiler_params=pltpu.CompilerParams(
            collective_id=0, has_side_effects=True, vmem_limit_bytes=48 * 1024 * 1024
        ),
        name="layer",
    )(*args)
    return pl.pallas_call(
        put_body,
        out_shape=tuple(jax.ShapeDtypeStruct(a.shape, a.dtype) for a in (residual, head_states)),
        in_specs=[pl.BlockSpec(memory_space=pltpu.VMEM)] * 2,
        out_specs=(pl.BlockSpec(memory_space=pltpu.HBM),) * 2,
        scratch_shapes=[dma((1 + pairs_dev * PUTS,))],
        compiler_params=pltpu.CompilerParams(vmem_limit_bytes=1024 * 1024),
        name="put",
    )(*results)


def solution(mesh):
    return jax.shard_map(
        per_device,
        mesh=mesh,
        in_specs=(
            P("grp", "ep"),
            P(("grp", "ep"), None, None),
            P(),
            P(None, "ep"),
            P(None, "ep"),
            P(None, "ep"),
            P(None, "ep"),
            P(),
            P(),
            P(),
            P(),
            P(None, "ep"),
            P(),
            P("grp", None),
            P("grp", None),
            P("grp", None),
            P("ep", None, None),
            P("ep", None, None),
            P("ep", None, None),
        ),
        out_specs=(P("grp", "ep"), P(("grp", "ep"), None, None)),
        check_vma=False,
    )
```

```python
import functools

import jax
import jax.numpy as jnp
from jax import lax
from jax.experimental import pallas as pl
from jax.experimental.pallas import tpu as pltpu
from jax.sharding import PartitionSpec as P

HEADS = 4
DK = 512
DV = 1024
GROUPS = 4

NORM_EPS = 1e-06
DECAY_TAU = 16.0
MESH = pl.DeviceIdType.MESH
F32 = jnp.float32
BF16 = jnp.bfloat16


def kernel_body(n, *refs):
    (
        residual,
        head_states,
        first_gain,
        w_query,
        w_key,
        w_value,
        w_gate,
        w_low,
        w_decay,
        decay_bias,
        head_gain,
        w_output,
        second_gain,
        routes,
        group_logits,
        expert_logits,
        expert_gate,
        expert_up,
        expert_down,
        layer_out,
        new_states,
        res_v,
        gain1_v,
        wq_v,
        wk_v,
        wv_v,
        wg_v,
        wlow_v,
        wdec_v,
        bias_v,
        hgain_v,
        wout_v,
        gain2_v,
        routes_v,
        glog_v,
        elog_v,
        eg_v,
        eu_v,
        ed_v,
        gath1,
        lhs,
        send2,
        recv2,
        cols,
        send3,
        gath3,
        stage3,
        gain1_f,
        gain2_f,
        stream_v,
        gath4,
        send5,
        recv5,
        local_sem,
        s1,
        r1,
        s2,
        r2,
        s3,
        r3,
        s4,
        r4,
        s5,
        r5,
    ) = refs
    states_v = new_states
    me = lax.axis_index("ep")
    seqs, own = residual.shape
    width = own * n
    pairs_dev = head_states.shape[0]
    dph = n // HEADS
    qw, vw = w_query.shape[1], w_value.shape[1]
    group_src = pairs_dev * dph
    my_seq = me * pairs_dev // HEADS
    my_head0 = lax.rem(me * pairs_dev, HEADS)
    src_head = me // dph
    tiles2 = send2.shape[1]
    rows3 = send3.shape[0]

    bit_count = n.bit_length() - 1
    signs = [1 - 2 * lax.rem(me // 2**b, 2) for b in range(bit_count)]

    def partner_of(o):
        if 2**bit_count != n:
            return lax.rem(me + o, n)
        return me + sum(signs[b] * 2**b for b in range(bit_count) if o >> b & 1)

    partner = [partner_of(o) for o in range(n)]
    far_first = range(n - 1, 0, -1)

    barrier = pltpu.get_barrier_semaphore()
    for o in far_first:
        pl.semaphore_signal(
            barrier, inc=1, device_id={"ep": partner[o]}, device_id_type=MESH
        )

    pieces = [
        (residual, res_v),
        (first_gain, gain1_v),
        (w_query, wq_v),
        (w_key, wk_v),
        (w_value, wv_v),
        (w_gate, wg_v),
        (w_low, wlow_v),
        (w_decay, wdec_v),
        (decay_bias, bias_v),
        (head_states, states_v),
        (head_gain, hgain_v),
        (w_output, wout_v),
        (second_gain, gain2_v),
        (routes, routes_v),
        (group_logits, glog_v),
        (expert_logits, elog_v),
        (expert_gate, eg_v),
        (expert_up, eu_v),
        (expert_down, ed_v),
    ]
    copies = [
        pltpu.make_async_copy(src, dst, local_sem.at[i]) for i, (src, dst) in enumerate(pieces)
    ]
    for copy in copies[:9]:
        copy.start()

    def staged(*indices):
        for i in indices:
            copies[i].wait()

    staged(0)
    pl.semaphore_wait(barrier, n - 1)

    def send(src, dst, send_sem, recv_sem, target):
        pltpu.make_async_remote_copy(
            src_ref=src,
            dst_ref=dst,
            send_sem=send_sem,
            recv_sem=recv_sem,
            device_id={"ep": target},
            device_id_type=MESH,
        ).start()

    def wait_blocks(buffer, sem):
        part = buffer.at[pl.ds(0, n - 1)]
        pltpu.make_async_copy(part, part, sem).wait()

    per = own // 128
    group_sizes = [4] * (n // 4 - 1) + [n % 4 + 2, 2]
    own_at = [pl.ds(pl.multiple_of(t * own, own), own) for t in partner]

    def absorb(gath, recv_sem, gains, weights, keep):
        accs = [jnp.zeros((seqs, w.shape[-1]), F32) for w in weights]
        total = jnp.zeros((seqs, own), F32)
        start = 0
        for size in group_sizes:
            some = range(start, start + size)
            start += size
            for o in some:
                if o:
                    block = gath.at[partner[o]]
                    pltpu.make_async_copy(block, block, recv_sem.at[partner[o]]).wait()
            for o in some:
                t = partner[o]
                x = gath[t].astype(F32)
                total = total + x * x
                gain = jnp.concatenate(
                    [gains[pl.ds(t * per + c, 1), :] for c in range(per)], axis=1
                )
                x = (x * gain).astype(BF16)
                if keep:
                    lhs[:, own_at[o]] = x
                accs = [
                    acc + jnp.dot(x, w[own_at[o], :], preferred_element_type=F32)
                    for acc, w in zip(accs, weights)
                ]
        scale = lax.rsqrt(jnp.sum(total, axis=1, keepdims=True) / width + NORM_EPS)
        return scale, [acc * scale for acc in accs]

    for o in far_first:
        send(res_v, gath1.at[me], s1.at[0], r1.at[me], partner[o])
    gath1[me] = res_v[...]
    staged(1)
    gain1_f[...] = gain1_v[...].astype(F32)
    staged(2, 3, 4, 5)
    for copy in copies[9:]:
        copy.start()
    scale1, (q, k, v, g) = absorb(gath1, r1, gain1_f, (wq_v, wk_v, wv_v, wg_v), True)
    row = jnp.concatenate([q, k, v, g], axis=1).astype(BF16).astype(F32)
    for c in range(tiles2):
        part = row[:, c * 128 : (c + 1) * 128]
        for s in range(seqs):
            send2[s, c : c + 1, :] = part[s : s + 1, :]

    my_slot = lax.rem(me, group_src)

    def target2(s):
        return (s * HEADS + src_head) // pairs_dev

    def copy2(s):
        return pltpu.make_async_remote_copy(
            src_ref=send2.at[s],
            dst_ref=recv2.at[my_slot],
            send_sem=s2.at[s],
            recv_sem=r2.at[my_slot],
            device_id={"ep": target2(s)},
            device_id_type=MESH,
        )

    @pl.loop(0, seqs)
    def _(s):
        @pl.when(target2(s) != me)
        def _():
            copy2(s).start()

        @pl.when(target2(s) == me)
        def _():
            pltpu.make_async_copy(send2.at[s], recv2.at[my_slot], r2.at[my_slot]).start()

    staged(6, 7, 8)
    low = scale1 * lax.dot_general(
        lhs[...], wlow_v[...], (((1,), (1,)), ((), ())), preferred_element_type=F32
    )
    head_at = pl.ds(pl.multiple_of(my_head0 * DK, DK), pairs_dev * DK)
    pre = jnp.dot(
        low,
        wdec_v[:, head_at].astype(F32),
        preferred_element_type=F32,
        precision=lax.Precision.HIGHEST,
    )
    row_is = lax.broadcasted_iota(jnp.int32, pre.shape, 0) == my_seq
    pre = jnp.sum(jnp.where(row_is, pre, 0.0), axis=0, keepdims=True) + bias_v[:, head_at]
    log_sig = jnp.minimum(pre, 0.0) - jnp.log(1.0 + jnp.exp(-jnp.abs(pre)))
    decay = jnp.exp(log_sig / DECAY_TAU)

    @pl.loop(0, group_src)
    def _(i):
        pltpu.make_async_copy(send2.at[0], recv2.at[i], r2.at[i]).wait()

    def lanes(i, start, size):
        out = []
        while size:
            c, off = start // 128, start % 128
            take = min(size, 128 - off)
            out.append(recv2[i, c : c + 1, :][:, off : off + take])
            start, size = start + take, size - take
        return out

    def gathered_row(p, start, size):
        out = []
        for i in range(dph):
            out.extend(lanes(p * dph + i, start, size))
        return jnp.concatenate(out, axis=1)

    def folded(row):
        return jnp.concatenate(
            [row[:, c * 128 : (c + 1) * 128] for c in range(row.shape[1] // 128)], axis=0
        )

    stack, overlap = [], []
    for p in range(pairs_dev):
        query = gathered_row(p, 0, qw) * DK ** (-0.5)
        key = gathered_row(p, qw, qw)
        fade = decay[:, p * DK : (p + 1) * DK]
        stack.extend([query * fade, key, fade])
        overlap.append(jnp.sum(query * key, axis=1, keepdims=True))
    stack.append(jnp.zeros((8 - len(stack), DK), F32))
    cols[...] = jnp.transpose(jnp.concatenate(stack, axis=0))
    values = [gathered_row(p, 2 * qw, vw) for p in range(pairs_dev)]
    staged(9, 10)
    step_rows = 128

    def read_step(i, accs):
        base = pl.multiple_of(i * step_rows, step_rows)
        out = []
        for p, acc in enumerate(accs):
            fading = cols[pl.ds(base, step_rows), 3 * p : 3 * p + 1]
            for r in range(0, step_rows, 8):
                acc = acc + states_v[p, pl.ds(base + r, 8), :] * fading[r : r + 8]
            out.append(acc)
        return tuple(out)

    zero = jnp.zeros((8, DV), F32)
    accs = lax.fori_loop(0, DK // step_rows, read_step, (zero,) * pairs_dev)
    mixed_rows = []
    for p in range(pairs_dev):
        read = jnp.sum(accs[p], axis=0, keepdims=True) + overlap[p] * values[p]
        scale = lax.rsqrt(jnp.mean(read * read, axis=1, keepdims=True) + NORM_EPS)
        read = folded(read)
        gate = folded(gathered_row(p, 2 * qw + vw, vw))
        mixed = read * scale * hgain_v[...].astype(F32) * (gate / (1.0 + jnp.exp(-gate)))
        mixed_rows.append(mixed)
    send3[...] = jnp.concatenate(mixed_rows, axis=0).astype(BF16)

    for o in far_first:
        send(send3, gath3.at[me], s3.at[0], r3.at[0], partner[o])
    gath3[me] = send3[...]

    @pl.loop(0, DK // step_rows)
    def _(i):
        base = pl.multiple_of(i * step_rows, step_rows)
        for p in range(pairs_dev):
            keys = cols[pl.ds(base, step_rows), 3 * p + 1 : 3 * p + 2]
            fades = cols[pl.ds(base, step_rows), 3 * p + 2 : 3 * p + 3]
            for r in range(0, step_rows, 8):
                at = pl.ds(base + r, 8)
                states_v[p, at, :] = (
                    states_v[p, at, :] * fades[r : r + 8] + keys[r : r + 8] * values[p]
                )

    staged(12, 13, 14, 15)
    gain2_f[...] = gain2_v[...].astype(F32)
    group_exp = jnp.exp(glog_v[...])
    group_prob = group_exp / jnp.sum(group_exp, axis=0, keepdims=True)
    route = routes_v[...]
    chosen = route[0:1, :] // (n // GROUPS)
    group_is = lax.broadcasted_iota(jnp.int32, group_prob.shape, 0) == chosen
    picked = jnp.sum(jnp.where(group_is, group_prob, 0.0), axis=0, keepdims=True)
    expert_exp = jnp.exp(elog_v[...])
    weights = expert_exp / jnp.sum(expert_exp, axis=0, keepdims=True) * picked
    mine = jnp.sum(jnp.where(route == me, weights, 0.0), axis=0, keepdims=True)
    diagonal = lax.broadcasted_iota(jnp.int32, (seqs, seqs), 0) == lax.broadcasted_iota(
        jnp.int32, (seqs, seqs), 1
    )
    mine = jnp.sum(jnp.where(diagonal, mine, 0.0), axis=1, keepdims=True)
    others3 = gath3.at[pl.ds(0, n - 1)]
    pltpu.make_async_copy(others3, others3, r3.at[0]).wait()
    per_seq = HEADS // pairs_dev
    for d in range(n):
        stage3[d // per_seq, (d % per_seq) * rows3 : (d % per_seq + 1) * rows3, :] = gath3[
            d
        ].astype(F32)
    for c in range(HEADS * DV // 128):
        lhs[:, c * 128 : (c + 1) * 128] = stage3[:, c, :].astype(BF16)
    staged(11)
    branch = jnp.dot(lhs[...], wout_v[...], preferred_element_type=F32)
    stream = (res_v[...].astype(F32) + branch.astype(BF16).astype(F32)).astype(BF16)
    stream_v[...] = stream

    for o in far_first:
        send(stream_v, gath4.at[me], s4.at[0], r4.at[me], partner[o])
    gath4[me] = stream
    staged(16, 17, 18)
    _, (gate_part, up_part) = absorb(gath4, r4, gain2_f, (eg_v.at[0], eu_v.at[0]), False)
    active = (gate_part / (1.0 + jnp.exp(-gate_part)) * up_part * mine).astype(BF16)

    def contribution(o):
        return jnp.dot(active, ed_v[0, :, own_at[o]], preferred_element_type=F32).astype(BF16)

    group = 8
    for first in range(n - 1, 0, -group):
        some = range(first, max(first - group, 0), -1)
        for o in some:
            send5[o] = contribution(o)
        for o in some:
            send(send5.at[o], recv5.at[me], s5.at[0], r5.at[0], partner[o])
    recv5[me] = contribution(0)
    wait_blocks(recv5, r5.at[0])
    total = jnp.zeros((seqs, own), F32)
    for s in range(n):
        total = total + recv5[s].astype(F32)
    layer_out[...] = (stream.astype(F32) + total).astype(BF16)

    wait_blocks(gath1, s1.at[0])
    wait_blocks(gath3, s3.at[0])
    wait_blocks(gath4, s4.at[0])
    wait_blocks(recv5, s5.at[0])

    @pl.loop(0, seqs)
    def _(s):
        @pl.when(target2(s) != me)
        def _():
            copy2(s).wait_send()


PUTS = 4


def put_body(layer_out, new_states, layer_hbm, states_hbm, sem):
    copies = [pltpu.make_async_copy(layer_out, layer_hbm, sem.at[0])]
    rows = DK // PUTS
    for p in range(new_states.shape[0]):
        for i in range(PUTS):
            at = pl.ds(i * rows, rows)
            copies.append(
                pltpu.make_async_copy(
                    new_states.at[p, at], states_hbm.at[p, at], sem.at[len(copies)]
                )
            )
    for copy in copies:
        copy.start()
    for copy in copies:
        copy.wait()


def per_device(*args):
    n = lax.axis_size("ep")
    args = list(args)
    for i in (2, 10, 12):
        args[i] = args[i].reshape(-1, 128)
    args[9] = args[9].reshape(1, -1)
    for i in (7, 13, 14, 15):
        args[i] = args[i].T
    args = [pltpu.with_memory_space_constraint(a, pltpu.HBM) for a in args]
    residual, head_states = args[0], args[1]
    seqs, own = residual.shape
    pairs_dev = head_states.shape[0]
    width = own * n
    qw, vw = args[3].shape[1], args[5].shape[1]
    group_src = pairs_dev * (n // HEADS)
    tiles2 = (2 * qw + 2 * vw) // 128
    rows3 = pairs_dev * DV // 128
    dma = pltpu.SemaphoreType.DMA
    stage = [pltpu.VMEM(a.shape, a.dtype) for i, a in enumerate(args) if i != 1]
    results = pl.pallas_call(
        functools.partial(kernel_body, n),
        out_shape=(
            pltpu.VMEM(residual.shape, BF16),
            pltpu.VMEM(head_states.shape, F32),
        ),
        in_specs=[pl.BlockSpec(memory_space=pltpu.HBM)] * len(args),
        out_specs=(pl.BlockSpec(memory_space=pltpu.VMEM),) * 2,
        scratch_shapes=stage
        + [
            pltpu.VMEM((n, seqs, own), BF16),
            pltpu.VMEM((seqs, width), BF16),
            pltpu.VMEM((seqs, tiles2, 128), F32),
            pltpu.VMEM((group_src, tiles2, 128), F32),
            pltpu.VMEM((DK, 8), F32),
            pltpu.VMEM((rows3, 128), BF16),
            pltpu.VMEM((n, rows3, 128), BF16),
            pltpu.VMEM((seqs, HEADS * DV // 128, 128), F32),
            pltpu.VMEM((width // 128, 128), F32),
            pltpu.VMEM((width // 128, 128), F32),
            pltpu.VMEM((seqs, own), BF16),
            pltpu.VMEM((n, seqs, own), BF16),
            pltpu.VMEM((n, seqs, own), BF16),
            pltpu.VMEM((n, seqs, own), BF16),
            dma((len(args),)),
            dma((1,)),
            dma((n,)),
            dma((seqs,)),
            dma((group_src,)),
            dma((1,)),
            dma((1,)),
            dma((1,)),
            dma((n,)),
            dma((1,)),
            dma((1,)),
        ],
        compiler_params=pltpu.CompilerParams(
            collective_id=0, has_side_effects=True, vmem_limit_bytes=48 * 1024 * 1024
        ),
        name="layer",
    )(*args)
    return pl.pallas_call(
        put_body,
        out_shape=tuple(jax.ShapeDtypeStruct(a.shape, a.dtype) for a in (residual, head_states)),
        in_specs=[pl.BlockSpec(memory_space=pltpu.VMEM)] * 2,
        out_specs=(pl.BlockSpec(memory_space=pltpu.HBM),) * 2,
        scratch_shapes=[dma((1 + pairs_dev * PUTS,))],
        compiler_params=pltpu.CompilerParams(vmem_limit_bytes=1024 * 1024),
        name="put",
    )(*results)


def solution(mesh):
    return jax.shard_map(
        per_device,
        mesh=mesh,
        in_specs=(
            P("grp", "ep"),
            P(("grp", "ep"), None, None),
            P(),
            P(None, "ep"),
            P(None, "ep"),
            P(None, "ep"),
            P(None, "ep"),
            P(),
            P(),
            P(),
            P(),
            P(None, "ep"),
            P(),
            P("grp", None),
            P("grp", None),
            P("grp", None),
            P("ep", None, None),
            P("ep", None, None),
            P("ep", None, None),
        ),
        out_specs=(P("grp", "ep"), P(("grp", "ep"), None, None)),
        check_vma=False,
    )
```
